32 devices in a mesh: fs: 8 (over z, y), tp: 4 (over x, core).
Axes of the slice: x: 2, y: 2, z: 4, core: 2. Of those that a mesh axis runs over, the one named last changes fastest.
Arguments:
- normed_input: bfloat16 [6144, 2048], P(('fs', 'tp')), may hold values from -6 to 6
- pre_act: bfloat16 [6144, 8192], P('fs', 'tp'), may hold values from -6 to 6
- out_grad: bfloat16 [6144, 2048], P(('fs', 'tp')), may hold values from -6 to 6
- up_weight: bfloat16 [2048, 8192], P('fs', 'tp'), may hold values from -0.125 to 0.125
- down_weight: bfloat16 [8192, 2048], P('tp', 'fs'), may hold values from -0.0625 to 0.0625
Outputs:
- input_grad: bfloat16 [6144, 2048], P(('fs', 'tp'))
- up_grad: float32 [2048, 8192], P('fs', 'tp')
- down_grad: float32 [8192, 2048], P('tp', 'fs')
The draws below stay inside these ranges and needn't reach their ends.
All inputs are finite; a program needn't handle non-finite values.
Results may differ from the reference program's by a relative error of at most 0.014.
Values may be sent and summed in bfloat16 or wider, within the bound.
A program may use at most 128 MiB of HBM per device.

```python
import jax
import jax.numpy as jnp
from jax import lax

D = 2048
FF = 8192
TOKENS = 6144
N_TP = 4


def raised(values, stream_key, source, target, blocks, factor):
    owner, partner = [(jnp.arange(values.shape[dim]) // (values.shape[dim] // blocks)).reshape([-1 if axis == dim else 1 for axis in range(values.ndim)]) for dim in (source, target)]
    chosen = jax.random.permutation(stream_key, blocks)[partner]
    strong = (owner == chosen) | (owner == (partner + blocks // 2) % blocks)
    return jnp.where(strong, factor * values, values)


def shard_levels(stream_key, extent, split, smallest, high):
    gain, own = 1.0, jax.random.fold_in(stream_key, 6)
    for position, shards_of in split:
        steps = jnp.exp(jax.random.uniform(jax.random.fold_in(own, position), (shards_of,), jnp.float32, smallest / len(split), high / len(split)))
        gain = gain * jnp.repeat(steps, extent[position] // shards_of).reshape([-1 if axis == position else 1 for axis in range(len(extent))])
    return gain


def centred(key, shape, scale, limit, cuts=(), dtype=jnp.bfloat16):
    drawn = jax.random.normal(key, shape, jnp.float32) * scale
    if len(cuts) > 0:
        drawn = shard_levels(key, shape, cuts, -0.22, 0.18) * drawn
    return jnp.clip(drawn, min=-limit, max=limit).astype(dtype)


def heavy_noise(stream_key, dims, spread, most, cuts, heavy, kind=jnp.bfloat16):
    result = spread * jax.random.normal(stream_key, dims, jnp.float32)
    if cuts:
        result = result * shard_levels(stream_key, dims, cuts, -0.22, 0.18)
    return jnp.clip(raised(result, jax.random.fold_in(stream_key, 3), *heavy), -most, most).astype(kind)


def setup_inputs(seed: int = 0) -> dict:
    streams_of = jax.random.split(jax.random.key(seed), 6)
    normed_input = centred(streams_of[0], (TOKENS, D), 1.0, 6.0, ((0, 32),))
    pre_act = centred(streams_of[1], (TOKENS, FF), 1.0, 6.0, ((0, 8), (1, 4)))
    out_grad = heavy_noise(streams_of[2], (TOKENS, D), 1.0, 6.0, ((0, 32),), (0, 1, 32, 2.75))
    up_weight = centred(streams_of[3], (D, FF), D ** -0.5, 0.125, ((0, 8), (1, 4)))
    down_weight = centred(streams_of[4], (FF, D), FF ** -0.5, 0.0625, ((0, 4), (1, 8)))
    return {"normed_input": normed_input, "pre_act": pre_act, "out_grad": out_grad, "up_weight": up_weight, "down_weight": down_weight}


def reference(normed_input, pre_act, out_grad, up_weight, down_weight):
    active = jnp.maximum(pre_act.astype(jnp.float32), 0.0)
    hidden = (active * active).astype(jnp.bfloat16)
    width = FF // N_TP
    up_blocks = up_weight.reshape(D, N_TP, width).transpose(1, 0, 2)
    down_blocks = down_weight.reshape(N_TP, width, D)
    act_blocks = active.reshape(TOKENS, N_TP, width).transpose(1, 0, 2)
    hid_blocks = hidden.reshape(TOKENS, N_TP, width).transpose(1, 0, 2)

    def one_block(items):
        up_part, down_part, act_part, hid_part = items
        grad_hidden = jnp.dot(out_grad, down_part.T, preferred_element_type=jnp.float32)
        pre_grad = (2.0 * act_part * grad_hidden).astype(jnp.bfloat16)
        part = jnp.dot(pre_grad, up_part.T, preferred_element_type=jnp.float32).astype(jnp.bfloat16)
        up_part_grad = jnp.dot(normed_input.T, pre_grad, preferred_element_type=jnp.float32)
        down_part_grad = jnp.dot(hid_part.T, out_grad, preferred_element_type=jnp.float32)
        return part, up_part_grad, down_part_grad

    parts, up_grads, down_grads = lax.map(one_block, (up_blocks, down_blocks, act_blocks, hid_blocks))
    input_grad = jnp.sum(parts.astype(jnp.float32), axis=0).astype(jnp.bfloat16)
    up_grad = up_grads.transpose(1, 0, 2).reshape(D, FF)
    down_grad = down_grads.reshape(FF, D)
    return input_grad, up_grad, down_grad
```

```python
import functools

import jax
import jax.numpy as jnp
from jax import lax
from jax.sharding import PartitionSpec as P

BF16, F32 = jnp.bfloat16, jnp.float32


def put(buffer, block, index, dim):
    return lax.dynamic_update_slice_in_dim(buffer, block, index * block.shape[dim], dim)


def take(buffer, index, size, dim):
    return lax.dynamic_slice_in_dim(buffer, index * size, size, dim)


class Grid:
    def __init__(self, fs, tp):
        self.ny = 2 if fs % 2 == 0 else 1
        self.nz = fs // self.ny
        self.nc = 2 if tp % 2 == 0 else 1
        self.nx = tp // self.nc
        f, t = lax.axis_index("fs"), lax.axis_index("tp")
        self.z, self.y = f // self.ny, f % self.ny
        self.x, self.c = t // self.nc, t % self.nc

    def shape_of(self, axis):
        return {
            "z": (self.nz, self.z, "fs", self.ny, self.ny),
            "y": (self.ny, self.y, "fs", 1, self.nz * self.ny),
            "x": (self.nx, self.x, "tp", self.nc, self.nc),
            "c": (self.nc, self.c, "tp", 1, self.nx * self.nc),
        }[axis]

    def pairs(self, axis, step, wrap):
        count, _, name, stride, _ = self.shape_of(axis)
        outer = (self.nz * self.ny if name == "fs" else self.nx * self.nc)
        result = []
        for device in range(outer):
            place = device // stride % count
            target = place + step
            if wrap:
                target %= count
            if 0 <= target < count:
                result.append((device, device + (target - place) * stride))
        return name, result

    def shift(self, value, axis, step, wrap=True):
        name, result = self.pairs(axis, step, wrap)
        return lax.ppermute(value, name, result)

    def arrange(self, pieces, axis, dim):
        count, place = self.shape_of(axis)[:2]
        if count == 2:
            first, second = pieces
            low = jnp.where(place == 0, first, second)
            high = jnp.where(place == 0, second, first)
            return jnp.concatenate([low, high], dim)
        shape = list(pieces[0].shape)
        shape[dim] *= count
        whole = jnp.zeros(shape, pieces[0].dtype)
        for k, piece in enumerate(pieces):
            whole = put(whole, piece, (place - k) % count, dim)
        return whole

    def gather(self, block, axis, dim):
        count = self.shape_of(axis)[0]
        pieces = [block] + [self.shift(block, axis, k) for k in range(1, count)]
        return self.arrange(pieces, axis, dim)

    def exchange(self, block, axis, cut, dim):
        count, place = self.shape_of(axis)[:2]
        size = block.shape[cut] // count
        pieces = [take(block, place, size, cut)]
        for k in range(1, count):
            piece = take(block, (place + k) % count, size, cut)
            pieces.append(self.shift(piece, axis, k))
        return self.arrange(pieces, axis, dim)

    def line_gather(self, block, dim):
        up, down = [block], [block]
        for _ in range(1, self.nz):
            up.append(self.shift(up[-1], "z", 1, False))
            down.append(self.shift(down[-1], "z", -1, False))
        return self.line_place(up, down, dim)

    def line_place(self, up, down, dim):
        shape = list(up[0].shape)
        shape[dim] *= self.nz
        whole = put(jnp.zeros(shape, up[0].dtype), up[0], self.z, dim)
        for k in range(1, self.nz):
            piece = jnp.where(self.z >= k, up[k], down[self.nz - k])
            whole = put(whole, piece, (self.z - k) % self.nz, dim)
        return whole

    def line_scatter(self, partial, dim):
        nz, size = self.nz, partial.shape[dim] // self.nz
        blocks = lax.optimization_barrier(
            tuple(take(partial, (self.z + k) % nz, size, dim) for k in range(nz))
        )
        total = blocks[0].astype(F32)
        arrived = {1: None, -1: None}
        for step in range(1, nz):
            for way in (1, -1):
                send = blocks[way * (nz - step) % nz]
                if arrived[way] is not None:
                    send = (send.astype(F32) + arrived[way].astype(F32)).astype(BF16)
                name, pairs = self.pairs("z", way, False)
                live = [
                    (a, b) for a, b in pairs
                    if 0 <= a // self.ny + way * (nz - step) < nz
                ]
                arrived[way] = lax.ppermute(send, name, live)
        for way in (1, -1):
            if arrived[way] is not None:
                total = total + arrived[way].astype(F32)
        return total

    def scatter(self, partial, axis, dim):
        count, place = self.shape_of(axis)[:2]
        size = partial.shape[dim] // count
        total = take(partial, place, size, dim).astype(F32)
        for k in range(1, count):
            piece = take(partial, (place + k) % count, size, dim)
            total = total + self.shift(piece, axis, k).astype(F32)
        return total.astype(BF16)


def local(fs, tp, normed_input, pre_act, out_grad, up_weight, down_weight):
    g = Grid(fs, tp)
    tokens, d = out_grad.shape
    half = tokens // 2

    def rows(block):
        block = block.reshape(1, 1, 1, tokens, d)
        block = g.gather(block, "y", 0)
        block = g.gather(block, "x", 1)
        return g.gather(block, "c", 2).reshape(-1, d)

    grad_rows = rows(out_grad)
    input_rows = rows(normed_input)
    acts = g.exchange(pre_act, "y", 1, 0)
    down_all = g.line_gather(g.exchange(down_weight, "y", 0, 1), 1)
    up_all = g.line_gather(g.exchange(up_weight, "y", 1, 0), 0)

    active = jnp.maximum(acts.astype(F32), 0.0)
    hidden = (active * active).astype(BF16)
    down_partial = lax.dot_general(
        hidden, grad_rows, (((0,), (0,)), ((), ())), preferred_element_type=F32
    ).astype(BF16)
    down_sum = g.line_scatter(down_partial, 1).astype(BF16)

    hidden_grad = lax.dot_general(
        grad_rows, down_all, (((1,), (1,)), ((), ())), preferred_element_type=F32
    )
    pre_grad = (2.0 * active * hidden_grad).astype(BF16)
    up_partial = lax.dot_general(
        input_rows, pre_grad, (((0,), (0,)), ((), ())), preferred_element_type=F32
    ).astype(BF16)
    up_sum = g.line_scatter(up_partial, 0).astype(BF16)

    part = lax.dot_general(
        pre_grad, up_all, (((1,), (1,)), ((), ())), preferred_element_type=F32
    ).astype(BF16)
    part = part.reshape(g.ny, g.nx, g.nc, tokens, d)
    part = g.scatter(part, "c", 2)
    one = g.scatter(g.scatter(part[..., :half, :], "x", 1), "y", 0)
    two = g.scatter(g.scatter(part[..., half:, :], "y", 0), "x", 1)
    input_grad = jnp.concatenate([one, two], 3).reshape(tokens, d)

    down_grad = g.exchange(down_sum, "y", 1, 0).astype(F32)
    up_grad = g.exchange(up_sum, "y", 0, 1).astype(F32)
    return input_grad, up_grad, down_grad


def solution(mesh):
    placed = (
        P(("fs", "tp"), None),
        P("fs", "tp"),
        P(("fs", "tp"), None),
        P("fs", "tp"),
        P("tp", "fs"),
    )
    return jax.shard_map(
        functools.partial(local, mesh.shape["fs"], mesh.shape["tp"]),
        mesh=mesh,
        in_specs=placed,
        out_specs=(P(("fs", "tp"), None), P("fs", "tp"), P("tp", "fs")),
        check_vma=False,
    )
```
